32 devices in a mesh: grp: 2 (over y), ep: 8 (over z, core), tp: 2 (over x).
Axes of the slice: x: 2, y: 2, z: 4, core: 2. Of those that a mesh axis runs over, the one named last changes fastest.
Arguments:
- tokens: bfloat16 [512, 2048], P(('grp', 'ep')), parts along dimension 0, may hold values from -12 to 12
- routes: int32 [512, 4], P(('grp', 'ep')), parts along dimension 0, may hold values from 0 to 7, all different within a row; in each aligned block of 32 rows (0 to 31, 32 to 63, ...) at most 32 rows name the same one
- gates: float32 [512, 4], P(('grp', 'ep')), parts along dimension 0, may hold values from 0.1 to 1
- norm_gain: bfloat16 [2048], replicated, may hold values from 0.099609375 to 1.8984375
- exp_gate: bfloat16 [8, 2048, 2048], P('ep', None, 'tp'), may hold values from -0.125 to 0.125
- exp_up: bfloat16 [8, 2048, 2048], P('ep', None, 'tp'), may hold values from -0.125 to 0.125
- exp_down: bfloat16 [8, 2048, 2048], P('ep', 'tp'), may hold values from -0.26516504 to 0.26516504
- sh_gate: bfloat16 [2048, 1024], P(None, 'tp'), may hold values from -0.125 to 0.125
- sh_up: bfloat16 [2048, 1024], P(None, 'tp'), may hold values from -0.125 to 0.125
- sh_down: bfloat16 [1024, 2048], P('tp'), may hold values from -0.375 to 0.375
- out_gain: bfloat16 [2048], P('tp'), may hold values from 0.099609375 to 1.8984375
Outputs:
- mixed: bfloat16 [512, 2048], P(('grp', 'ep'), 'tp'), parts along dimension 0
The draws below stay inside these ranges and needn't reach their ends.
There are 2 independent parts, one for each index of `grp`. The reference program is written for one: setup_inputs(seed, part) draws one part's arguments, and reference() takes and returns one part's arrays. A program takes and returns all parts, laid end to end along the dimension named above; an argument that names none is the same for every part. Nothing has to cross between parts.
Inputs may be any that keep to these rules, and one draw needn't show every extreme that they name: `routes`: each row names 4 different experts; within the rows of one device (aligned blocks of 32 rows) no expert is named by more than 32 rows, a bound that some block reaches.
All inputs are finite; a program needn't handle non-finite values.
Results may differ from the reference program's by a relative error of at most 0.015.
Values may be sent and summed in bfloat16 or wider, within the bound.
A program may use at most 64 MiB of HBM per device.

```python
import math
import jax
import jax.numpy as jnp
import numpy as np
from jax import lax

D = 2048
FF = 2048
SHARED_FF = 1024
TOP_K = 4
TOK_EP = 32
EXPERTS = 8
TOKENS = 256
CAP = 32
N_EP = 8
N_TP = 2


def rising_down(key, array_shape, fan_in):
    column = jnp.arange(D, dtype=jnp.float32) / (D - 1)
    base_draw = jnp.clip(jax.random.normal(key, array_shape, jnp.float32), -4.0, 4.0)
    profile = 5.0 ** (column - 0.5)
    return (base_draw * profile * fan_in ** (-0.5)).astype(jnp.bfloat16)


def draw_exp_down(key, part):
    return rising_down(jax.random.fold_in(key, 11), (EXPERTS, FF, D), FF)


def draw_sh_down(key, part):
    return rising_down(jax.random.fold_in(key, 23), (SHARED_FF, D), SHARED_FF)


def shard_levels(own_key, extent, cuts, least, top_value):
    def one(dim, blocks):
        heights = jax.random.uniform(jax.random.fold_in(jax.random.fold_in(own_key, 6), dim), (blocks,), jnp.float32, least / len(cuts), top_value / len(cuts))
        return jnp.repeat(jnp.exp(heights), extent[dim] // blocks).reshape((-1,) + (1,) * (len(extent) - dim - 1))

    factor_of = one(*cuts[0])
    for cut in cuts[1:]:
        factor_of = factor_of * one(*cut)
    return factor_of


def shared_out(rng, own, number, rows, amount, top, most, skew):
    ranking = jax.random.permutation(rng, amount)
    packed, usual = load_shares(amount, rows * top, most, skew, True), load_shares(amount, rows * top, most, skew, False)
    places = jnp.arange(amount)

    def named(sizes, rotation):
        used = int((sizes > 0).sum())
        fixed = max(1, used // 4)
        moved = fixed + (places - fixed + rotation * (used - fixed)) % max(1, amount - fixed)
        return jnp.zeros((amount,), jnp.int32).at[ranking[jnp.where(places < fixed, places, moved)]].set(jnp.asarray(sizes, jnp.int32))

    sizes = jnp.where(number % 4 == 0, named(packed, number // 4), named(usual, number - number // 4 - 1))
    mixed = jax.random.permutation(jax.random.fold_in(own, 3), amount)
    giver, receiver = mixed[0:amount // 2 * 2:2], mixed[1:amount // 2 * 2:2]
    margin = jnp.minimum(sizes[giver] - 1, most - sizes[receiver]) // 2
    margin = jnp.where((giver == ranking[0]) | (receiver == ranking[0]) | (sizes[receiver] == 0), 0, jnp.maximum(margin, 0))
    moved = jax.random.randint(jax.random.fold_in(own, 4), (amount // 2,), 0, 1 << 20) % (margin + 1)
    sizes = sizes.at[giver].add(-moved).at[receiver].add(moved)
    labels = jnp.searchsorted(jnp.cumsum(sizes), jnp.arange(rows * top), side="right").astype(jnp.int32)
    listing = labels.reshape(top, rows).T
    listing = listing[jax.random.permutation(jax.random.fold_in(own, 1), rows)]
    rotation = jax.random.randint(jax.random.fold_in(own, 2), (rows, 1), 0, top)
    return jnp.take_along_axis(listing, (jnp.arange(top)[None, :] + rotation) % top, axis=1)


def load_shares(count, total, reach, slope, full):
    portions = [(1 << 20) // math.isqrt(standing ** slope) + 1 for standing in range(1, count + 1)]
    largest = reach if full else min(reach, max(-(-total // count), total * portions[0] // sum(portions)))
    least = 1 if total - largest >= count - 1 else 0
    given, surplus = [largest] + [least] * (count - 1), total - largest - least * (count - 1)
    while surplus > 0:
        movable = [i for i in range(1, count) if given[i] < largest] or [i for i in range(1, count) if given[i] < reach]
        pool, budget = sum([portions[i] for i in movable]), surplus
        for i in movable:
            extra = min(reach - given[i], max(1, budget * portions[i] // pool), surplus)
            given[i] = given[i] + extra
            surplus = surplus - extra
    return np.array(given)


def normal_values(stream_key, dims, scale, reach, cuts=(), held_as=jnp.bfloat16):
    result = jax.random.normal(stream_key, dims, jnp.float32) * scale
    if len(cuts) > 0:
        result = shard_levels(stream_key, dims, cuts, -0.22, 0.18) * result
    return jnp.clip(result, min=-reach, max=reach).astype(held_as)


def setup_inputs(seed: int = 0, part: int = 0) -> dict:
    seeds = jax.random.split(jax.random.key(seed), 12)
    part_keys = jax.random.split(jax.random.fold_in(seeds[11], part), 12)
    tokens = normal_values(part_keys[0], (TOKENS, D), 2.0, 12.0, ((0, 8),))
    routes_keys = jax.random.split(jax.random.fold_in(part_keys[1], 1), TOKENS // TOK_EP)
    routes_turns = jax.random.permutation(jax.random.fold_in(part_keys[1], 3), TOKENS // TOK_EP)
    routes = jax.vmap(lambda own, number: shared_out(jax.random.fold_in(part_keys[1], 2), own, number, TOK_EP, EXPERTS, TOP_K, CAP, 2))(routes_keys, routes_turns).reshape((TOKENS, TOP_K))
    gates = jnp.clip(jnp.exp(math.log(1.0) - 2.3025851 * jax.random.uniform(part_keys[2], (TOKENS, TOP_K), jnp.float32) ** shard_levels(part_keys[2], (TOKENS, TOP_K), ((0, 8),), -0.2, 0.2)), 0.1, 1.0)
    norm_gain = jnp.clip(1.0 + 0.18 * jax.random.normal(seeds[3], (D,), jnp.float32), 0.099609375, 1.8984375).astype(jnp.bfloat16)
    exp_gate = normal_values(seeds[4], (EXPERTS, D, FF), D ** -0.5, 0.125, ((0, 8), (2, 2)))
    exp_up = normal_values(seeds[5], (EXPERTS, D, FF), D ** -0.5, 0.125, ((0, 8), (2, 2)))
    exp_down = draw_exp_down(jax.random.fold_in(seeds[11], 71), part)
    sh_gate = normal_values(seeds[7], (D, SHARED_FF), D ** -0.5, 0.125, ((1, 2),))
    sh_up = normal_values(seeds[8], (D, SHARED_FF), D ** -0.5, 0.125, ((1, 2),))
    sh_down = draw_sh_down(jax.random.fold_in(seeds[11], 71), part)
    out_gain = jnp.clip(1.0 + 0.18 * jax.random.normal(seeds[10], (D,), jnp.float32), 0.099609375, 1.8984375).astype(jnp.bfloat16)
    return {"tokens": tokens, "routes": routes, "gates": gates, "norm_gain": norm_gain, "exp_gate": exp_gate, "exp_up": exp_up, "exp_down": exp_down, "sh_gate": sh_gate, "sh_up": sh_up, "sh_down": sh_down, "out_gain": out_gain}


EPSILON = 1e-06

def slot_order(flat_routes, count):
    hits = (flat_routes[:, None] == jnp.arange(count, dtype=jnp.int32)[None, :]).astype(jnp.int32)
    before = jnp.cumsum(hits, axis=0) - hits
    return lax.optimization_barrier(jnp.sum(before * hits, axis=1)).astype(jnp.int32)

def swiglu_blocks(row_block, w_gate, w_up, w_down):
    gate_act = jnp.dot(row_block, w_gate, preferred_element_type=jnp.float32)
    up_act = jnp.dot(row_block, w_up, preferred_element_type=jnp.float32)
    hidden = (jax.nn.silu(gate_act) * up_act).astype(jnp.bfloat16)
    width = w_down.shape[0] // N_TP
    pieces = jnp.einsum('rnf,nfd->nrd', hidden.astype(jnp.float32).reshape(row_block.shape[0], N_TP, width), w_down.astype(jnp.float32).reshape(N_TP, width, w_down.shape[1]))
    rounded = lax.optimization_barrier(pieces.astype(jnp.bfloat16)).astype(jnp.float32)
    return lax.optimization_barrier(jnp.sum(rounded, axis=0)).astype(jnp.bfloat16)

def reference(tokens, routes, gates, norm_gain, exp_gate, exp_up, exp_down, sh_gate, sh_up, sh_down, out_gain):
    values = tokens.astype(jnp.float32)
    normed = (values * lax.rsqrt(lax.optimization_barrier(jnp.mean(values * values, axis=1, keepdims=True)) + EPSILON) * norm_gain.astype(jnp.float32)).astype(jnp.bfloat16)
    flat_expert = routes.reshape(-1).astype(jnp.int32)
    slot_index = jax.vmap(lambda block_routes: slot_order(block_routes, EXPERTS))(routes.reshape(N_EP, TOK_EP * TOP_K).astype(jnp.int32)).reshape(-1)
    flat_token = jnp.repeat(jnp.arange(TOKENS, dtype=jnp.int32), TOP_K)
    source = flat_token // TOK_EP
    position = flat_expert * (N_EP * CAP) + source * CAP + slot_index
    token_table = jnp.zeros((EXPERTS * N_EP * CAP,), jnp.int32).at[position].set(flat_token)
    weight_table = jnp.zeros((EXPERTS * N_EP * CAP,), jnp.float32).at[position].set(gates.reshape(-1))

    def one_expert(inputs):
        token_index, w_gate, w_up, w_down = inputs
        return swiglu_blocks(normed[token_index], w_gate, w_up, w_down)
    outputs = lax.map(one_expert, (token_table.reshape(EXPERTS, N_EP * CAP), exp_gate, exp_up, exp_down))
    routed = jnp.zeros((TOKENS, D), jnp.float32).at[token_table].add(weight_table[:, None] * outputs.reshape(-1, D).astype(jnp.float32))
    shared = swiglu_blocks(normed, sh_gate, sh_up, sh_down).astype(jnp.float32)
    total = routed + shared
    scale = lax.rsqrt(lax.optimization_barrier(jnp.mean(total * total, axis=1, keepdims=True)) + EPSILON)
    return (total * scale * out_gain.astype(jnp.float32)).astype(jnp.bfloat16)
```

```python
import functools

import jax
import jax.numpy as jnp
from jax import lax
from jax.experimental import pallas as pl
from jax.experimental.pallas import tpu as pltpu
from jax.sharding import PartitionSpec as P

EPSILON = 1e-06
MESH = pl.DeviceIdType.MESH
F32 = jnp.float32
BF16 = jnp.bfloat16


def silu(v):
    return v / (1.0 + jnp.exp(-v))


def kernel(
    n_ep, n_tp, experts,
    tok_ref, routes_ref, gates_ref, ngain_ref, wg_hbm, wu_hbm, wd_hbm, sg_hbm, su_hbm, sd_hbm, ogain_ref,
    out_ref,
    wg, wu, wd, sg, su, sd, xs, hid, shid, shp, d_out, d_in, x_out, x_in, acc, z_out, z_in, q_out, q_in,
    w_sem, disp_send, disp_recv, fwd_send, fwd_recv, d_send, d_recv, x_send, x_recv, z_send, z_recv, q_send, q_recv,
):
    nz = n_ep // 2
    me = lax.axis_index("ep")
    t = lax.axis_index("tp")
    z, c = me // 2, lax.rem(me, 2)
    other = 1 - c
    T, D = tok_ref.shape
    F = wg.shape[1]
    S = sg.shape[1]
    Dt = D // n_tp
    rows = nz * T
    pad = xs.shape[3] - D

    loads = []
    for i, (src, dst) in enumerate(
        ((sg_hbm, sg), (su_hbm, su), (sd_hbm, sd), (wg_hbm.at[0], wg), (wu_hbm.at[0], wu), (wd_hbm.at[0], wd))
    ):
        copy = pltpu.make_async_copy(src, dst, w_sem.at[i])
        copy.start()
        loads.append(copy)

    def zpeer(dz):
        return lax.rem(z + dz, nz)

    def tpeer(j):
        return lax.rem(t + j, n_tp)

    partner = {"ep": z * 2 + other}
    barrier = pltpu.get_barrier_semaphore()
    peers = [{"ep": zpeer(dz) * 2 + c} for dz in range(1, nz)] + [partner]
    peers += [{"tp": tpeer(j)} for j in range(1, n_tp)]
    for peer in peers:
        pl.semaphore_signal(barrier, inc=1, device_id=peer, device_id_type=MESH)

    def remote(src, dst, ssem, rsem, device):
        return pltpu.make_async_remote_copy(
            src_ref=src, dst_ref=dst, send_sem=ssem, recv_sem=rsem, device_id=device, device_id_type=MESH
        )

    values = tok_ref[...].astype(F32)
    scale = lax.rsqrt(jnp.mean(values * values, axis=1, keepdims=True) + EPSILON)
    normed = (values * scale * ngain_ref[...].astype(F32)).astype(BF16)
    lane = lax.broadcasted_iota(jnp.int32, (T, pad), 1)
    lane_expert = lax.rem(lane, experts)
    dense = jnp.zeros((T, pad), F32)
    for k in range(routes_ref.shape[1]):
        dense = dense + jnp.where(lane_expert == routes_ref[:, k : k + 1], gates_ref[:, k : k + 1], 0.0)
    high = dense.astype(BF16).astype(F32)
    rest = dense - high
    mid = rest.astype(BF16).astype(F32)
    part = lane // experts
    packed = jnp.where(part == 0, high, jnp.where(part == 1, mid, jnp.where(part == 2, rest - mid, 0.0)))
    xs[c, z, :, :D] = normed
    xs[c, z, :, D:] = packed.astype(BF16)

    pl.semaphore_wait(barrier, len(peers))

    own = xs.at[c, z]
    sends = []
    order = sorted(range(1, nz), key=lambda d: -min(d, nz - d))
    for dz in order:
        copy = remote(own, own, disp_send.at[dz], disp_recv.at[dz], {"ep": zpeer(dz) * 2 + c})
        copy.start()
        sends.append(copy)
    first = remote(own, own, fwd_send.at[0], fwd_recv.at[0], partner)
    first.start()

    loads[0].wait()
    loads[1].wait()
    tile = min(256, S)

    @pl.loop(0, S // tile)
    def _(i):
        cols = pl.ds(pl.multiple_of(i * tile, tile), tile)
        x = xs[c, z, :, :D]
        g = jnp.dot(x, sg[:, cols], preferred_element_type=F32)
        u = jnp.dot(x, su[:, cols], preferred_element_type=F32)
        shid[:, cols] = (silu(g) * u).astype(BF16)

    loads[2].wait()
    dtile = min(256, Dt)

    @pl.loop(0, D // dtile)
    def _(i):
        cols = pl.ds(pl.multiple_of(i * dtile, dtile), dtile)
        shp[:, cols] = jnp.dot(shid[...], sd[:, cols], preferred_element_type=F32)

    forwards = [first]
    for dz in range(1, nz):
        src_z = lax.rem(z - dz + nz, nz)
        block = xs.at[c, src_z]
        remote(block, block, disp_send.at[dz], disp_recv.at[dz], partner).wait_recv()
        copy = remote(block, block, fwd_send.at[dz], fwd_recv.at[dz], partner)
        copy.start()
        forwards.append(copy)

    loads[3].wait()
    loads[4].wait()
    ftile = min(256, F)
    glane = lax.broadcasted_iota(jnp.int32, (rows, pad), 1)
    mine = (lax.rem(glane, experts) == me) & (glane < 3 * experts)

    def hidden(half, slot):
        packed_gates = xs[half, :, :, D:].reshape(rows, pad).astype(F32)
        weight = jnp.sum(jnp.where(mine, packed_gates, 0.0), axis=1, keepdims=True)

        @pl.loop(0, F // ftile)
        def _(i):
            cols = pl.ds(pl.multiple_of(i * ftile, ftile), ftile)
            x = xs[half, :, :, :D].reshape(rows, D)
            g = jnp.dot(x, wg[:, cols], preferred_element_type=F32)
            u = jnp.dot(x, wu[:, cols], preferred_element_type=F32)
            hid[slot, :, cols] = (silu(g) * u * weight).astype(BF16)

    hidden(c, 0)
    for dz in range(nz):
        src_z = lax.rem(z - dz + nz, nz)
        block = xs.at[other, src_z]
        remote(block, block, fwd_send.at[dz], fwd_recv.at[dz], partner).wait_recv()
    hidden(other, 1)
    loads[5].wait()

    def down(slot, tp, store):
        @pl.loop(0, Dt // dtile)
        def _(i):
            src = pl.ds(pl.multiple_of(tp * Dt + i * dtile, dtile), dtile)
            dst = pl.ds(pl.multiple_of(i * dtile, dtile), dtile)
            store(src, dst, jnp.dot(hid[slot], wd[:, src], preferred_element_type=F32))

    js = list(range(1, n_tp)) + [0]
    d_copies = {}
    for j in js:
        def store(src, dst, value):
            d_out[j, :, :, dst] = value.astype(BF16).reshape(nz, T, dtile)

        down(1, tpeer(j), store)
        copy = remote(d_out.at[j], d_in.at[j], d_send.at[j], d_recv.at[j], partner)
        copy.start()
        d_copies[j] = copy

    x_copies = {}
    for j in js:
        def keep(src, dst, value):
            acc[:, :, dst] = value.reshape(nz, T, dtile)
            acc[z, :, dst] += shp[:, src]

        down(0, tpeer(j), keep)
        d_copies[j].wait_recv()
        if j == 0:
            acc[...] += d_in[j].astype(F32)
        else:
            for dz in order + [0]:
                zt = zpeer(dz)
                x_out[j, zt] = (acc[zt] + d_in[j, zt].astype(F32)).astype(BF16)
                copy = remote(
                    x_out.at[j, zt], x_in.at[j, zt], x_send.at[j, dz], x_recv.at[j, dz], {"tp": tpeer(j)}
                )
                copy.start()
                x_copies[j, dz] = copy

    z_copies = {}
    for dz in order + [0]:
        zt = zpeer(dz)
        total = acc[zt]
        for j in range(1, n_tp):
            x_copies[j, dz].wait_recv()
            total = total + x_in[j, zt].astype(F32)
        if dz == 0:
            acc[zt] = total
        else:
            z_out[dz] = total.astype(BF16)
            copy = remote(z_out.at[dz], z_in.at[dz], z_send.at[dz], z_recv.at[dz], {"ep": zt * 2 + c})
            copy.start()
            z_copies[dz] = copy

    total = acc[z]
    for dz in range(1, nz):
        z_copies[dz].wait_recv()
        total = total + z_in[dz].astype(F32)
    squares = jnp.sum(total * total, axis=1, keepdims=True)
    q_out[...] = jnp.broadcast_to(squares, q_out.shape)
    q_copies = []
    for j in range(1, n_tp):
        copy = remote(q_out, q_in.at[j], q_send.at[j], q_recv.at[j], {"tp": tpeer(j)})
        copy.start()
        q_copies.append(copy)
    gained = total * ogain_ref[...].astype(F32)
    for j, copy in enumerate(q_copies):
        copy.wait_recv()
        squares = squares + q_in[j + 1, :, :1]
    out_ref[...] = (gained * lax.rsqrt(squares / D + EPSILON)).astype(BF16)

    for copy in sends + forwards + list(d_copies.values()) + list(x_copies.values()) + list(z_copies.values()) + q_copies:
        copy.wait_send()


def solution(mesh):
    n_ep, n_tp = mesh.shape["ep"], mesh.shape["tp"]
    nz = n_ep // 2

    def shards(tokens, routes, gates, norm_gain, exp_gate, exp_up, exp_down, sh_gate, sh_up, sh_down, out_gain):
        T, D = tokens.shape
        local, _, F = exp_gate.shape
        S = sh_gate.shape[1]
        assert local == 1
        experts = local * n_ep
        Dt = D // n_tp
        pad = 128 * ((3 * experts + 127) // 128)
        vmem = pl.BlockSpec(memory_space=pltpu.VMEM)
        hbm = pl.BlockSpec(memory_space=pl.ANY)
        dma = pltpu.SemaphoreType.DMA
        return pl.pallas_call(
            functools.partial(kernel, n_ep, n_tp, experts),
            out_shape=jax.ShapeDtypeStruct((T, Dt), BF16),
            in_specs=[vmem] * 4 + [hbm] * 6 + [vmem],
            out_specs=vmem,
            scratch_shapes=[
                pltpu.VMEM((D, F), BF16),
                pltpu.VMEM((D, F), BF16),
                pltpu.VMEM((F, D), BF16),
                pltpu.VMEM((D, S), BF16),
                pltpu.VMEM((D, S), BF16),
                pltpu.VMEM((S, D), BF16),
                pltpu.VMEM((2, nz, T, D + pad), BF16),
                pltpu.VMEM((2, nz * T, F), BF16),
                pltpu.VMEM((T, S), BF16),
                pltpu.VMEM((T, D), F32),
                pltpu.VMEM((n_tp, nz, T, Dt), BF16),
                pltpu.VMEM((n_tp, nz, T, Dt), BF16),
                pltpu.VMEM((n_tp, nz, T, Dt), BF16),
                pltpu.VMEM((n_tp, nz, T, Dt), BF16),
                pltpu.VMEM((nz, T, Dt), F32),
                pltpu.VMEM((nz, T, Dt), BF16),
                pltpu.VMEM((nz, T, Dt), BF16),
                pltpu.VMEM((T, 128), F32),
                pltpu.VMEM((n_tp, T, 128), F32),
                dma((6,)),
                dma((nz,)), dma((nz,)), dma((nz,)), dma((nz,)),
                dma((n_tp,)), dma((n_tp,)),
                dma((n_tp, nz)), dma((n_tp, nz)),
                dma((nz,)), dma((nz,)),
                dma((n_tp,)), dma((n_tp,)),
            ],
            compiler_params=pltpu.CompilerParams(collective_id=0, has_side_effects=True),
        )(
            tokens, routes, gates, norm_gain.reshape(1, -1), exp_gate, exp_up, exp_down,
            sh_gate, sh_up, sh_down, out_gain.reshape(1, -1),
        )

    placed = (
        P(("grp", "ep"), None),
        P(("grp", "ep"), None),
        P(("grp", "ep"), None),
        P(),
        P("ep", None, "tp"),
        P("ep", None, "tp"),
        P("ep", "tp", None),
        P(None, "tp"),
        P(None, "tp"),
        P("tp", None),
        P("tp"),
    )
    return jax.shard_map(
        shards, mesh=mesh, in_specs=placed, out_specs=P(("grp", "ep"), "tp"), check_vma=False
    )
```

```python
import functools

import jax
import jax.numpy as jnp
from jax import lax
from jax.experimental import pallas as pl
from jax.experimental.pallas import tpu as pltpu
from jax.sharding import PartitionSpec as P

EPSILON = 1e-06
MESH = pl.DeviceIdType.MESH
F32 = jnp.float32
BF16 = jnp.bfloat16


def silu(v):
    return v / (1.0 + jnp.exp(-v))


def kernel(
    n_ep, n_tp, experts,
    tok_ref, routes_ref, gates_ref, ngain_ref, wg_hbm, wu_hbm, wd_hbm, sg_hbm, su_hbm, sd_hbm, ogain_ref,
    out_ref,
    wg, wu, wd, sg, su, sd, xs, hid, shid, shp, d_out, d_in, x_out, x_in, acc, z_out, z_in, q_out, q_in,
    w_sem, disp_send, disp_recv, fwd_send, fwd_recv, d_send, d_recv, x_send, x_recv, z_send, z_recv, q_send, q_recv,
):
    nz = n_ep // 2
    me = lax.axis_index("ep")
    t = lax.axis_index("tp")
    z, c = me // 2, lax.rem(me, 2)
    other = 1 - c
    T, D = tok_ref.shape
    F = wg.shape[1]
    S = sg.shape[1]
    Dt = D // n_tp
    rows = nz * T
    pad = xs.shape[3] - D

    loads = []
    for i, (src, dst) in enumerate(
        ((sg_hbm, sg), (su_hbm, su), (sd_hbm, sd), (wg_hbm.at[0], wg), (wu_hbm.at[0], wu), (wd_hbm.at[0], wd))
    ):
        copy = pltpu.make_async_copy(src, dst, w_sem.at[i])
        copy.start()
        loads.append(copy)

    def zpeer(dz):
        peer = z
        for bit in range(dz.bit_length()):
            if dz >> bit & 1:
                peer = peer + (1 << bit) * (1 - 2 * lax.rem(z // (1 << bit), 2))
        return peer

    def tpeer(j):
        return lax.rem(t + j, n_tp)

    partner = {"ep": z * 2 + other}
    barrier = pltpu.get_barrier_semaphore()
    peers = [{"ep": zpeer(dz) * 2 + c} for dz in range(1, nz)] + [partner]
    peers += [{"tp": tpeer(j)} for j in range(1, n_tp)]
    for peer in peers:
        pl.semaphore_signal(barrier, inc=1, device_id=peer, device_id_type=MESH)

    def remote(src, dst, ssem, rsem, device):
        return pltpu.make_async_remote_copy(
            src_ref=src, dst_ref=dst, send_sem=ssem, recv_sem=rsem, device_id=device, device_id_type=MESH
        )

    values = tok_ref[...].astype(F32)
    scale = lax.rsqrt(jnp.mean(values * values, axis=1, keepdims=True) + EPSILON)
    normed = (values * scale * ngain_ref[...].astype(F32).reshape(1, D)).astype(BF16)
    row = lax.broadcasted_iota(jnp.int32, (pad, T), 0)
    row_expert = lax.rem(row, experts)
    dense = jnp.zeros((pad, T), F32)
    for k in range(routes_ref.shape[0]):
        dense = dense + jnp.where(row_expert == routes_ref[k : k + 1, :], gates_ref[k : k + 1, :], 0.0)
    high = dense.astype(BF16).astype(F32)
    rest = dense - high
    mid = rest.astype(BF16).astype(F32)
    part = row // experts
    packed = jnp.where(part == 0, high, jnp.where(part == 1, mid, jnp.where(part == 2, rest - mid, 0.0)))
    packed = packed.T
    xs[c, z, :, :D] = normed
    xs[c, z, :, D:] = packed.astype(BF16)

    pl.semaphore_wait(barrier, len(peers))

    own = xs.at[c, z]
    sends = []
    order = list(range(nz - 1, 0, -1))
    for dz in order:
        copy = remote(own, own, disp_send.at[dz], disp_recv.at[dz], {"ep": zpeer(dz) * 2 + c})
        copy.start()
        sends.append(copy)
    first = remote(own, own, fwd_send.at[0], fwd_recv.at[0], partner)
    first.start()

    loads[0].wait()
    loads[1].wait()
    tile = min(256, S)

    @pl.loop(0, S // tile)
    def _(i):
        cols = pl.ds(pl.multiple_of(i * tile, tile), tile)
        x = xs[c, z, :, :D]
        g = jnp.dot(x, sg[:, cols], preferred_element_type=F32)
        u = jnp.dot(x, su[:, cols], preferred_element_type=F32)
        shid[:, cols] = (silu(g) * u).astype(BF16)

    loads[2].wait()
    dtile = min(256, Dt)

    @pl.loop(0, D // dtile)
    def _(i):
        cols = pl.ds(pl.multiple_of(i * dtile, dtile), dtile)
        shp[:, cols] = jnp.dot(shid[...], sd[:, cols], preferred_element_type=F32)

    forwards = [first]
    for dz in range(1, nz):
        src_z = zpeer(dz)
        block = xs.at[c, src_z]
        remote(block, block, disp_send.at[dz], disp_recv.at[dz], partner).wait_recv()
        copy = remote(block, block, fwd_send.at[dz], fwd_recv.at[dz], partner)
        copy.start()
        forwards.append(copy)

    loads[3].wait()
    loads[4].wait()
    ftile = min(256, F)
    glane = lax.broadcasted_iota(jnp.int32, (rows, pad), 1)
    mine = (lax.rem(glane, experts) == me) & (glane < 3 * experts)

    def hidden(half, slot):
        packed_gates = xs[half, :, :, D:].reshape(rows, pad).astype(F32)
        weight = jnp.sum(jnp.where(mine, packed_gates, 0.0), axis=1, keepdims=True)

        @pl.loop(0, F // ftile)
        def _(i):
            cols = pl.ds(pl.multiple_of(i * ftile, ftile), ftile)
            x = xs[half, :, :, :D].reshape(rows, D)
            g = jnp.dot(x, wg[:, cols], preferred_element_type=F32)
            u = jnp.dot(x, wu[:, cols], preferred_element_type=F32)
            hid[slot, :, cols] = (silu(g) * u * weight).astype(BF16)

    hidden(c, 0)
    for dz in range(nz):
        src_z = zpeer(dz)
        block = xs.at[other, src_z]
        remote(block, block, fwd_send.at[dz], fwd_recv.at[dz], partner).wait_recv()
    hidden(other, 1)
    loads[5].wait()

    def down(slot, tp, store):
        @pl.loop(0, Dt // dtile)
        def _(i):
            src = pl.ds(pl.multiple_of(tp * Dt + i * dtile, dtile), dtile)
            dst = pl.ds(pl.multiple_of(i * dtile, dtile), dtile)
            store(src, dst, jnp.dot(hid[slot], wd[:, src], preferred_element_type=F32))

    js = list(range(1, n_tp)) + [0]
    d_copies = {}
    for j in js:
        def store(src, dst, value):
            d_out[j, :, :, dst] = value.astype(BF16).reshape(nz, T, dtile)

        down(1, tpeer(j), store)
        copy = remote(d_out.at[j], d_in.at[j], d_send.at[j], d_recv.at[j], partner)
        copy.start()
        d_copies[j] = copy

    x_copies = {}
    for j in js:
        def keep(src, dst, value):
            acc[:, :, dst] = value.reshape(nz, T, dtile)
            acc[z, :, dst] += shp[:, src]

        down(0, tpeer(j), keep)
        d_copies[j].wait_recv()
        if j == 0:
            acc[...] += d_in[j].astype(F32)
        else:
            for dz in order + [0]:
                zt = zpeer(dz)
                x_out[j, zt] = (acc[zt] + d_in[j, zt].astype(F32)).astype(BF16)
                copy = remote(
                    x_out.at[j, zt], x_in.at[j, zt], x_send.at[j, dz], x_recv.at[j, dz], {"tp": tpeer(j)}
                )
                copy.start()
                x_copies[j, dz] = copy

    z_copies = {}
    for dz in order + [0]:
        zt = zpeer(dz)
        total = acc[zt]
        for j in range(1, n_tp):
            x_copies[j, dz].wait_recv()
            total = total + x_in[j, zt].astype(F32)
        if dz == 0:
            acc[zt] = total
        else:
            z_out[dz] = total.astype(BF16)
            copy = remote(z_out.at[dz], z_in.at[dz], z_send.at[dz], z_recv.at[dz], {"ep": zt * 2 + c})
            copy.start()
            z_copies[dz] = copy

    total = acc[z]
    for dz in range(1, nz):
        z_copies[dz].wait_recv()
        total = total + z_in[dz].astype(F32)
    squares = jnp.sum(total * total, axis=1, keepdims=True)
    q_out[...] = jnp.broadcast_to(squares, q_out.shape)
    q_copies = []
    for j in range(1, n_tp):
        copy = remote(q_out, q_in.at[j], q_send.at[j], q_recv.at[j], {"tp": tpeer(j)})
        copy.start()
        q_copies.append(copy)
    gained = total * ogain_ref[...].astype(F32).reshape(1, Dt)
    for j, copy in enumerate(q_copies):
        copy.wait_recv()
        squares = squares + q_in[j + 1, :, :1]
    out_ref[...] = (gained * lax.rsqrt(squares / D + EPSILON)).astype(BF16)

    for copy in sends + forwards + list(d_copies.values()) + list(x_copies.values()) + list(z_copies.values()) + q_copies:
        copy.wait_send()


def solution(mesh):
    n_ep, n_tp = mesh.shape["ep"], mesh.shape["tp"]
    nz = n_ep // 2

    def shards(tokens, routes, gates, norm_gain, exp_gate, exp_up, exp_down, sh_gate, sh_up, sh_down, out_gain):
        T, D = tokens.shape
        local, _, F = exp_gate.shape
        S = sh_gate.shape[1]
        assert local == 1
        experts = local * n_ep
        Dt = D // n_tp
        pad = 128 * ((3 * experts + 127) // 128)
        vmem = pl.BlockSpec(memory_space=pltpu.VMEM)
        hbm = pl.BlockSpec(memory_space=pl.ANY)
        dma = pltpu.SemaphoreType.DMA
        return pl.pallas_call(
            functools.partial(kernel, n_ep, n_tp, experts),
            out_shape=jax.ShapeDtypeStruct((T, Dt), BF16),
            in_specs=[vmem] * 4 + [hbm] * 6 + [vmem],
            out_specs=vmem,
            scratch_shapes=[
                pltpu.VMEM((D, F), BF16),
                pltpu.VMEM((D, F), BF16),
                pltpu.VMEM((F, D), BF16),
                pltpu.VMEM((D, S), BF16),
                pltpu.VMEM((D, S), BF16),
                pltpu.VMEM((S, D), BF16),
                pltpu.VMEM((2, nz, T, D + pad), BF16),
                pltpu.VMEM((2, nz * T, F), BF16),
                pltpu.VMEM((T, S), BF16),
                pltpu.VMEM((T, D), F32),
                pltpu.VMEM((n_tp, nz, T, Dt), BF16),
                pltpu.VMEM((n_tp, nz, T, Dt), BF16),
                pltpu.VMEM((n_tp, nz, T, Dt), BF16),
                pltpu.VMEM((n_tp, nz, T, Dt), BF16),
                pltpu.VMEM((nz, T, Dt), F32),
                pltpu.VMEM((nz, T, Dt), BF16),
                pltpu.VMEM((nz, T, Dt), BF16),
                pltpu.VMEM((T, 128), F32),
                pltpu.VMEM((n_tp, T, 128), F32),
                dma((6,)),
                dma((nz,)), dma((nz,)), dma((nz,)), dma((nz,)),
                dma((n_tp,)), dma((n_tp,)),
                dma((n_tp, nz)), dma((n_tp, nz)),
                dma((nz,)), dma((nz,)),
                dma((n_tp,)), dma((n_tp,)),
            ],
            compiler_params=pltpu.CompilerParams(collective_id=0, has_side_effects=True),
        )(
            tokens, routes.T, gates.T, norm_gain, exp_gate, exp_up, exp_down,
            sh_gate, sh_up, sh_down, out_gain,
        )

    placed = (
        P(("grp", "ep"), None),
        P(("grp", "ep"), None),
        P(("grp", "ep"), None),
        P(),
        P("ep", None, "tp"),
        P("ep", None, "tp"),
        P("ep", "tp", None),
        P(None, "tp"),
        P(None, "tp"),
        P("tp", None),
        P("tp"),
    )
    return jax.shard_map(
        shards, mesh=mesh, in_specs=placed, out_specs=P(("grp", "ep"), "tp"), check_vma=False
    )
```

```python
import functools

import jax
import jax.numpy as jnp
from jax import lax
from jax.experimental import pallas as pl
from jax.experimental.pallas import tpu as pltpu
from jax.sharding import PartitionSpec as P

EPSILON = 1e-06
MESH = pl.DeviceIdType.MESH
F32 = jnp.float32
BF16 = jnp.bfloat16


def silu(v):
    return v / (1.0 + jnp.exp(-v))


def kernel(
    n_ep, n_tp, experts,
    tok_ref, routes_ref, gates_ref, ngain_ref, wg_hbm, wu_hbm, wd_hbm, sg_hbm, su_hbm, sd_hbm, ogain_ref,
    out_ref,
    wg, wu, wd, sg, su, sd, xs, hid, shid, shp, d_out, d_in, x_out, x_in, acc, z_out, z_in, q_out, q_in,
    w_sem, disp_send, disp_recv, fwd_send, fwd_recv, d_send, d_recv, x_send, x_recv, z_send, z_recv, q_send, q_recv,
):
    nz = n_ep // 2
    me = lax.axis_index("ep")
    t = lax.axis_index("tp")
    z, c = me // 2, lax.rem(me, 2)
    other = 1 - c
    T, D = tok_ref.shape
    F = wg.shape[1]
    S = sg.shape[1]
    Dt = D // n_tp
    rows = nz * T
    pad = xs.shape[3] - D

    loads = []
    for i, (src, dst) in enumerate(
        ((sg_hbm, sg), (su_hbm, su), (sd_hbm, sd), (wg_hbm.at[0], wg), (wu_hbm.at[0], wu), (wd_hbm.at[0], wd))
    ):
        copy = pltpu.make_async_copy(src, dst, w_sem.at[i])
        copy.start()
        loads.append(copy)

    def zpeer(dz):
        peer = z
        for bit in range(dz.bit_length()):
            if dz >> bit & 1:
                peer = peer + (1 << bit) * (1 - 2 * lax.rem(z // (1 << bit), 2))
        return peer

    def tpeer(j):
        return lax.rem(t + j, n_tp)

    partner = {"ep": z * 2 + other}
    barrier = pltpu.get_barrier_semaphore()
    peers = [{"ep": zpeer(dz) * 2 + c} for dz in range(1, nz)] + [partner]
    peers += [{"tp": tpeer(j)} for j in range(1, n_tp)]
    for peer in peers:
        pl.semaphore_signal(barrier, inc=1, device_id=peer, device_id_type=MESH)

    def remote(src, dst, ssem, rsem, device):
        return pltpu.make_async_remote_copy(
            src_ref=src, dst_ref=dst, send_sem=ssem, recv_sem=rsem, device_id=device, device_id_type=MESH
        )

    values = tok_ref[...].astype(F32)
    scale = lax.rsqrt(jnp.mean(values * values, axis=1, keepdims=True) + EPSILON)
    normed = (values * scale * ngain_ref[...].astype(F32).reshape(1, D)).astype(BF16)
    row = lax.broadcasted_iota(jnp.int32, (pad, T), 0)
    row_expert = lax.rem(row, experts)
    dense = jnp.zeros((pad, T), F32)
    for k in range(routes_ref.shape[0]):
        dense = dense + jnp.where(row_expert == routes_ref[k : k + 1, :], gates_ref[k : k + 1, :], 0.0)
    high = dense.astype(BF16).astype(F32)
    rest = dense - high
    mid = rest.astype(BF16).astype(F32)
    part = row // experts
    packed = jnp.where(part == 0, high, jnp.where(part == 1, mid, jnp.where(part == 2, rest - mid, 0.0)))
    packed = packed.T
    xs[c, z, :, :D] = normed
    xs[c, z, :, D:] = packed.astype(BF16)

    pl.semaphore_wait(barrier, len(peers))

    own = xs.at[c, z]
    sends = []
    order = list(range(nz - 1, 0, -1))
    for dz in order:
        copy = remote(own, own, disp_send.at[dz], disp_recv.at[dz], {"ep": zpeer(dz) * 2 + c})
        copy.start()
        sends.append(copy)
    first = remote(own, own, fwd_send.at[0], fwd_recv.at[0], partner)
    first.start()

    loads[0].wait()
    loads[1].wait()
    tile = min(256, S)

    @pl.loop(0, S // tile)
    def _(i):
        cols = pl.ds(pl.multiple_of(i * tile, tile), tile)
        x = xs[c, z, :, :D]
        g = jnp.dot(x, sg[:, cols], preferred_element_type=F32)
        u = jnp.dot(x, su[:, cols], preferred_element_type=F32)
        shid[:, cols] = (silu(g) * u).astype(BF16)

    loads[2].wait()
    dtile = min(512, Dt)

    @pl.loop(0, D // dtile)
    def _(i):
        cols = pl.ds(pl.multiple_of(i * dtile, dtile), dtile)
        shp[:, cols] = jnp.dot(shid[...], sd[:, cols], preferred_element_type=F32)

    forwards = [first]
    for dz in range(1, nz):
        src_z = zpeer(dz)
        block = xs.at[c, src_z]
        remote(block, block, disp_send.at[dz], disp_recv.at[dz], partner).wait_recv()
        copy = remote(block, block, fwd_send.at[dz], fwd_recv.at[dz], partner)
        copy.start()
        forwards.append(copy)

    loads[3].wait()
    loads[4].wait()
    ftile = min(512, F)
    glane = lax.broadcasted_iota(jnp.int32, (rows, pad), 1)
    mine = (lax.rem(glane, experts) == me) & (glane < 3 * experts)

    def hidden(half, slot):
        packed_gates = xs[half, :, :, D:].reshape(rows, pad).astype(F32)
        weight = jnp.sum(jnp.where(mine, packed_gates, 0.0), axis=1, keepdims=True)

        @pl.loop(0, F // ftile)
        def _(i):
            cols = pl.ds(pl.multiple_of(i * ftile, ftile), ftile)
            x = xs[half, :, :, :D].reshape(rows, D)
            g = jnp.dot(x, wg[:, cols], preferred_element_type=F32)
            u = jnp.dot(x, wu[:, cols], preferred_element_type=F32)
            hid[slot, :, cols] = (silu(g) * u * weight).astype(BF16)

    hidden(c, 0)
    for dz in range(nz):
        src_z = zpeer(dz)
        block = xs.at[other, src_z]
        remote(block, block, fwd_send.at[dz], fwd_recv.at[dz], partner).wait_recv()
    hidden(other, 1)
    loads[5].wait()

    def down(slot, tp, store):
        @pl.loop(0, Dt // dtile)
        def _(i):
            src = pl.ds(pl.multiple_of(tp * Dt + i * dtile, dtile), dtile)
            dst = pl.ds(pl.multiple_of(i * dtile, dtile), dtile)
            store(src, dst, jnp.dot(hid[slot], wd[:, src], preferred_element_type=F32))

    js = list(range(1, n_tp)) + [0]
    d_copies = {}
    x_copies = {}
    for j in js:
        def store(src, dst, value):
            d_out[j, :, :, dst] = value.astype(BF16).reshape(nz, T, dtile)

        down(1, tpeer(j), store)
        copy = remote(d_out.at[j], d_in.at[j], d_send.at[j], d_recv.at[j], partner)
        copy.start()
        d_copies[j] = copy

        def keep(src, dst, value):
            acc[:, :, dst] = value.reshape(nz, T, dtile)
            acc[z, :, dst] += shp[:, src]

        down(0, tpeer(j), keep)
        d_copies[j].wait_recv()
        if j == 0:
            acc[...] += d_in[j].astype(F32)
        else:
            for dz in order + [0]:
                zt = zpeer(dz)
                x_out[j, zt] = (acc[zt] + d_in[j, zt].astype(F32)).astype(BF16)
                copy = remote(
                    x_out.at[j, zt], x_in.at[j, zt], x_send.at[j, dz], x_recv.at[j, dz], {"tp": tpeer(j)}
                )
                copy.start()
                x_copies[j, dz] = copy

    z_copies = {}
    for dz in order + [0]:
        zt = zpeer(dz)
        total = acc[zt]
        for j in range(1, n_tp):
            x_copies[j, dz].wait_recv()
            total = total + x_in[j, zt].astype(F32)
        if dz == 0:
            acc[zt] = total
        else:
            z_out[dz] = total.astype(BF16)
            copy = remote(z_out.at[dz], z_in.at[dz], z_send.at[dz], z_recv.at[dz], {"ep": zt * 2 + c})
            copy.start()
            z_copies[dz] = copy

    total = acc[z]
    for dz in range(1, nz):
        z_copies[dz].wait_recv()
        total = total + z_in[dz].astype(F32)
    squares = jnp.sum(total * total, axis=1, keepdims=True)
    q_out[...] = jnp.broadcast_to(squares, q_out.shape)
    q_copies = []
    for j in range(1, n_tp):
        copy = remote(q_out, q_in.at[j], q_send.at[j], q_recv.at[j], {"tp": tpeer(j)})
        copy.start()
        q_copies.append(copy)
    gained = total * ogain_ref[...].astype(F32).reshape(1, Dt)
    for j, copy in enumerate(q_copies):
        copy.wait_recv()
        squares = squares + q_in[j + 1, :, :1]
    out_ref[...] = (gained * lax.rsqrt(squares / D + EPSILON)).astype(BF16)

    for copy in sends + forwards + list(d_copies.values()) + list(x_copies.values()) + list(z_copies.values()) + q_copies:
        copy.wait_send()


def solution(mesh):
    n_ep, n_tp = mesh.shape["ep"], mesh.shape["tp"]
    nz = n_ep // 2

    def shards(tokens, routes, gates, norm_gain, exp_gate, exp_up, exp_down, sh_gate, sh_up, sh_down, out_gain):
        T, D = tokens.shape
        local, _, F = exp_gate.shape
        S = sh_gate.shape[1]
        assert local == 1
        experts = local * n_ep
        Dt = D // n_tp
        pad = 128 * ((3 * experts + 127) // 128)
        vmem = pl.BlockSpec(memory_space=pltpu.VMEM)
        hbm = pl.BlockSpec(memory_space=pl.ANY)
        dma = pltpu.SemaphoreType.DMA
        return pl.pallas_call(
            functools.partial(kernel, n_ep, n_tp, experts),
            out_shape=jax.ShapeDtypeStruct((T, Dt), BF16),
            in_specs=[vmem] * 4 + [hbm] * 6 + [vmem],
            out_specs=vmem,
            scratch_shapes=[
                pltpu.VMEM((D, F), BF16),
                pltpu.VMEM((D, F), BF16),
                pltpu.VMEM((F, D), BF16),
                pltpu.VMEM((D, S), BF16),
                pltpu.VMEM((D, S), BF16),
                pltpu.VMEM((S, D), BF16),
                pltpu.VMEM((2, nz, T, D + pad), BF16),
                pltpu.VMEM((2, nz * T, F), BF16),
                pltpu.VMEM((T, S), BF16),
                pltpu.VMEM((T, D), F32),
                pltpu.VMEM((n_tp, nz, T, Dt), BF16),
                pltpu.VMEM((n_tp, nz, T, Dt), BF16),
                pltpu.VMEM((n_tp, nz, T, Dt), BF16),
                pltpu.VMEM((n_tp, nz, T, Dt), BF16),
                pltpu.VMEM((nz, T, Dt), F32),
                pltpu.VMEM((nz, T, Dt), BF16),
                pltpu.VMEM((nz, T, Dt), BF16),
                pltpu.VMEM((T, 128), F32),
                pltpu.VMEM((n_tp, T, 128), F32),
                dma((6,)),
                dma((nz,)), dma((nz,)), dma((nz,)), dma((nz,)),
                dma((n_tp,)), dma((n_tp,)),
                dma((n_tp, nz)), dma((n_tp, nz)),
                dma((nz,)), dma((nz,)),
                dma((n_tp,)), dma((n_tp,)),
            ],
            compiler_params=pltpu.CompilerParams(collective_id=0, has_side_effects=True),
        )(
            tokens, routes.T, gates.T, norm_gain, exp_gate, exp_up, exp_down,
            sh_gate, sh_up, sh_down, out_gain,
        )

    placed = (
        P(("grp", "ep"), None),
        P(("grp", "ep"), None),
        P(("grp", "ep"), None),
        P(),
        P("ep", None, "tp"),
        P("ep", None, "tp"),
        P("ep", "tp", None),
        P(None, "tp"),
        P(None, "tp"),
        P("tp", None),
        P("tp"),
    )
    return jax.shard_map(
        shards, mesh=mesh, in_specs=placed, out_specs=P(("grp", "ep"), "tp"), check_vma=False
    )
```
